32 devices in a mesh: grp: 2 (over y), ep: 4 (over z), tp: 4 (over x, core).
Axes of the slice: x: 2, y: 2, z: 4, core: 2. Of those that a mesh axis runs over, the one named last changes fastest.
Arguments:
- conv_x: bfloat16 [8192, 2048], P(('grp', 'ep', 'tp')), parts along dimension 0, may hold values from -6 to 6
- conv_c: bfloat16 [8192, 2048], P(('grp', 'ep', 'tp')), parts along dimension 0, may hold values from -6 to 6
- conv_b: bfloat16 [8192, 2048], P(('grp', 'ep', 'tp')), parts along dimension 0, may hold values from -6 to 6
- conv_taps: float32 [3, 2048], replicated, may hold values from -3.5 to 3.5
- w_out: bfloat16 [2048, 2048], P('tp'), may hold values from -0.125 to 0.125
- tokens_b: bfloat16 [4096, 2048], P(('grp', 'ep', 'tp')), parts along dimension 0, may hold values from -6 to 6
- norm_gain: float32 [2048], replicated, may hold values from 0.1 to 1.9
- route_b: int32 [4096, 2], P(('grp', 'ep', 'tp')), parts along dimension 0, may hold values from 0 to 3, all different within a row; in each aligned block of 128 rows (0 to 127, 128 to 255, ...) at most 128 rows name the same one
- route_weights: float32 [4096, 2], P(('grp', 'ep', 'tp')), parts along dimension 0, may hold values from 0.1 to 1
- w_gate: bfloat16 [4, 2048, 1024], P('ep', None, 'tp'), may hold values from -0.125 to 0.125
- w_up: bfloat16 [4, 2048, 1024], P('ep', None, 'tp'), may hold values from -0.125 to 0.125
- w_down: bfloat16 [4, 1024, 2048], P('ep', 'tp'), may hold values from -0.1875 to 0.1875
Outputs:
- mixed_a: bfloat16 [8192, 2048], P(('grp', 'ep', 'tp')), parts along dimension 0
- experts_b: bfloat16 [4096, 2048], P(('grp', 'ep', 'tp')), parts along dimension 0
The draws below stay inside these ranges and needn't reach their ends.
There are 2 independent parts, one for each index of `grp`. The reference program is written for one: setup_inputs(seed, part) draws one part's arguments, and reference() takes and returns one part's arrays. A program takes and returns all parts, laid end to end along the dimension named above; an argument that names none is the same for every part. Nothing has to cross between parts.
Inputs may be any that keep to these rules, and one draw needn't show every extreme that they name: `route_b`: the 2 experts of a row differ. Within the 128 rows of one device no expert is named more than 128 times, and in every draw some device names some expert exactly 128 times.
All inputs are finite; a program needn't handle non-finite values.
Results may differ from the reference program's by a relative error of at most 0.012.
Values may be sent and summed in bfloat16 or wider, within the bound.
No kernel may reach another device: no remote copies, remote signals or barrier semaphores. Data moves between devices by JAX's collectives and lax.ppermute only.
A program may use at most 128 MiB of HBM per device.

```python
import math
import jax
import jax.numpy as jnp
import numpy as np
from jax import lax

D = 2048
CH = 2048
CONV = 3
FF = 1024
TOPK = 2
ROWS_B = 128
EXPERTS = 4
CAP = 128
SEQ = 4096
TOKENS_B = 2048
N_EP = 4
N_TP = 4


def steps_of(stream_key, shape, cuts, low, high):
    factor_of = 1.0
    for axis_at, blocks in cuts:
        draws = jax.random.uniform(jax.random.fold_in(jax.random.fold_in(stream_key, 6), axis_at), (blocks,), jnp.float32, low / len(cuts), high / len(cuts))
        factor_of = factor_of * jnp.repeat(jnp.exp(draws), shape[axis_at] // blocks).reshape((-1,) + (1,) * (len(shape) - 1 - axis_at))
    return factor_of


def assign_block(stream_key, own, number, rows, count, top, bound, slope):
    sequence = jax.random.permutation(stream_key, count)
    heavy_load, usual = portions_of(count, rows * top, bound, slope, True), portions_of(count, rows * top, bound, slope, False)
    places = jnp.arange(count)

    def named(tallies, offset_by):
        used = int((tallies > 0).sum())
        fixed = max(1, used // 4)
        shifted = fixed + (places - fixed + offset_by * (used - fixed)) % max(1, count - fixed)
        return jnp.zeros((count,), jnp.int32).at[sequence[jnp.where(places < fixed, places, shifted)]].set(jnp.asarray(tallies, jnp.int32))

    tallies = jnp.where(number % 4 == 0, named(heavy_load, number // 4), named(usual, number - number // 4 - 1))
    mixed = jax.random.permutation(jax.random.fold_in(own, 3), count)
    giver, sink = mixed[0:count // 2 * 2:2], mixed[1:count // 2 * 2:2]
    slack = jnp.minimum(tallies[giver] - 1, bound - tallies[sink]) // 2
    slack = jnp.where((giver == sequence[0]) | (sink == sequence[0]) | (tallies[sink] == 0), 0, jnp.maximum(slack, 0))
    shifted = jax.random.randint(jax.random.fold_in(own, 4), (count // 2,), 0, 1 << 20) % (slack + 1)
    tallies = tallies.at[giver].add(-shifted).at[sink].add(shifted)
    members = jnp.searchsorted(jnp.cumsum(tallies), jnp.arange(rows * top), side="right").astype(jnp.int32)
    table = members.reshape(top, rows).T
    table = table[jax.random.permutation(jax.random.fold_in(own, 1), rows)]
    offset_by = jax.random.randint(jax.random.fold_in(own, 2), (rows, 1), 0, top)
    return jnp.take_along_axis(table, (jnp.arange(top)[None, :] + offset_by) % top, axis=1)


def portions_of(count, total, most, lean, full):
    weights = [(1 << 20) // math.isqrt(standing ** lean) + 1 for standing in range(1, count + 1)]
    largest = most if full else min(most, max(-(-total // count), total * weights[0] // sum(weights)))
    least = 1 if total - largest >= count - 1 else 0
    counts, rest = [largest] + [least] * (count - 1), total - largest - least * (count - 1)
    while rest > 0:
        candidates = [i for i in range(1, count) if counts[i] < largest] or [i for i in range(1, count) if counts[i] < most]
        mass, left = sum([weights[i] for i in candidates]), rest
        for i in candidates:
            addition = min(most - counts[i], max(1, left * weights[i] // mass), rest)
            counts[i] = counts[i] + addition
            rest = rest - addition
    return np.array(counts)


def bell_draw(key, dims, spread, most, cuts=(), kind=jnp.bfloat16):
    entries = spread * jax.random.normal(key, dims, jnp.float32)
    if cuts:
        entries = entries * steps_of(key, dims, cuts, -0.22, 0.18)
    return jnp.clip(entries, -most, most).astype(kind)


def setup_inputs(seed: int = 0, part: int = 0) -> dict:
    streams_of = jax.random.split(jax.random.key(seed), 13)
    own_keys = jax.random.split(jax.random.fold_in(streams_of[12], part), 13)
    conv_x = bell_draw(own_keys[0], (SEQ, CH), 1.0, 6.0, ((0, 16),))
    conv_c = bell_draw(own_keys[1], (SEQ, CH), 1.0, 6.0, ((0, 16),))
    conv_b = bell_draw(own_keys[2], (SEQ, CH), 1.0, 6.0, ((0, 16),))
    conv_taps = bell_draw(streams_of[3], (CONV, CH), CONV ** -0.5, 3.5, (), jnp.float32)
    w_out = bell_draw(streams_of[4], (CH, D), CH ** -0.5, 0.125, ((0, 4),))
    tokens_b = bell_draw(own_keys[5], (TOKENS_B, D), 1.0, 6.0, ((0, 16),))
    norm_gain = jnp.clip(1.0 + 0.18 * jax.random.normal(streams_of[6], (D,), jnp.float32), 0.1, 1.9)
    route_b_keys = jax.random.split(jax.random.fold_in(own_keys[7], 1), TOKENS_B // ROWS_B)
    route_b_turns = jax.random.permutation(jax.random.fold_in(own_keys[7], 3), TOKENS_B // ROWS_B)
    route_b = jax.vmap(lambda own, number: assign_block(jax.random.fold_in(own_keys[7], 2), own, number, ROWS_B, EXPERTS, TOPK, CAP, 2))(route_b_keys, route_b_turns).reshape((TOKENS_B, TOPK))
    route_weights = jnp.clip(jnp.exp(math.log(1.0) - 2.3025851 * jax.random.uniform(own_keys[8], (TOKENS_B, TOPK), jnp.float32) ** steps_of(own_keys[8], (TOKENS_B, TOPK), ((0, 16),), -0.2, 0.2)), 0.1, 1.0)
    w_gate = bell_draw(streams_of[9], (EXPERTS, D, FF), D ** -0.5, 0.125, ((0, 4), (2, 4)))
    w_up = bell_draw(streams_of[10], (EXPERTS, D, FF), D ** -0.5, 0.125, ((0, 4), (2, 4)))
    w_down = bell_draw(streams_of[11], (EXPERTS, FF, D), FF ** -0.5, 0.1875, ((0, 4), (1, 4)))
    return {"conv_x": conv_x, "conv_c": conv_c, "conv_b": conv_b, "conv_taps": conv_taps, "w_out": w_out, "tokens_b": tokens_b, "norm_gain": norm_gain, "route_b": route_b, "route_weights": route_weights, "w_gate": w_gate, "w_up": w_up, "w_down": w_down}


def slot_ranks(route):
    flat = route.reshape(-1)
    onehot = (flat[:, None] == jnp.arange(EXPERTS, dtype=jnp.int32)[None, :]).astype(jnp.int32)
    earlier = jnp.cumsum(onehot, axis=0) - onehot
    return lax.optimization_barrier(jnp.sum(earlier * onehot, axis=1)).reshape(route.shape)

def reference(conv_x, conv_c, conv_b, conv_taps, w_out, tokens_b, norm_gain, route_b, route_weights, w_gate, w_up, w_down):
    mixed_u = (conv_c.astype(jnp.float32) * conv_x.astype(jnp.float32)).astype(jnp.bfloat16)
    extended = jnp.concatenate([jnp.zeros((CONV - 1, CH), jnp.bfloat16), mixed_u], axis=0)
    filtered = jnp.zeros((SEQ, CH), jnp.float32)
    for shift_tap in range(CONV):
        filtered = filtered + conv_taps[shift_tap][None, :] * extended[shift_tap:shift_tap + SEQ].astype(jnp.float32)
    gated = (conv_b.astype(jnp.float32) * filtered).astype(jnp.bfloat16)
    mixed_a = jnp.dot(gated, w_out, preferred_element_type=jnp.float32).astype(jnp.bfloat16)
    tokens_f = tokens_b.astype(jnp.float32)
    normed = (tokens_f * lax.rsqrt(lax.optimization_barrier(jnp.mean(tokens_f * tokens_f, axis=-1, keepdims=True)) + 1e-06) * norm_gain).astype(jnp.bfloat16)
    sources = N_EP * N_TP
    slots = jax.vmap(slot_ranks)(route_b.reshape(sources, ROWS_B, TOPK)).reshape(TOKENS_B, TOPK)
    source_id = (jnp.arange(TOKENS_B, dtype=jnp.int32) // ROWS_B)[:, None]
    position = source_id * CAP + slots
    token_id = jnp.broadcast_to(jnp.arange(TOKENS_B, dtype=jnp.int32)[:, None], (TOKENS_B, TOPK))
    fill_table = jnp.full((EXPERTS, sources * CAP), TOKENS_B, jnp.int32)
    fill_table = fill_table.at[route_b.reshape(-1), position.reshape(-1)].set(token_id.reshape(-1))
    padded = jnp.concatenate([normed, jnp.zeros((1, D), jnp.bfloat16)], axis=0)

    def one_expert(operands):
        fill_row, gate_w, up_w, down_w = operands
        rows = padded[fill_row]
        gate_val = jnp.dot(rows, gate_w, preferred_element_type=jnp.float32)
        up_val = jnp.dot(rows, up_w, preferred_element_type=jnp.float32)
        hidden = (jax.nn.silu(gate_val) * up_val).astype(jnp.bfloat16)
        blocks = hidden.reshape(-1, N_TP, FF // N_TP).astype(jnp.float32)
        down_blocks = down_w.reshape(N_TP, FF // N_TP, D).astype(jnp.float32)
        partial_sums = jnp.einsum('rqf,qfd->qrd', blocks, down_blocks).astype(jnp.bfloat16)
        partial_sums = lax.optimization_barrier(partial_sums)
        return lax.optimization_barrier(jnp.sum(partial_sums.astype(jnp.float32), axis=0)).astype(jnp.bfloat16)
    results = lax.map(one_expert, (fill_table, w_gate, w_up, w_down))
    flat_results = results.reshape(EXPERTS * sources * CAP, D)
    picked = flat_results[route_b * (sources * CAP) + position]
    shares = route_weights / lax.optimization_barrier(jnp.sum(route_weights, axis=-1, keepdims=True))
    experts_b = lax.optimization_barrier(jnp.sum(picked.astype(jnp.float32) * shares[:, :, None], axis=1)).astype(jnp.bfloat16)
    return (mixed_a, experts_b)
```

```python
import jax
import jax.numpy as jnp
from jax import lax
from jax.sharding import PartitionSpec as P

D = 2048
TOPK = 2


def shifted(x, axis, by):
    size = lax.axis_size(axis)
    pairs = [(i, i + by) for i in range(size) if 0 <= i + by < size]
    return lax.ppermute(x, axis, pairs)


def slot_targets(route, experts, capacity):
    flat = route.reshape(-1)
    onehot = (flat[:, None] == jnp.arange(experts, dtype=jnp.int32)[None, :]).astype(jnp.int32)
    earlier = jnp.cumsum(onehot, axis=0) - onehot
    ranks = jnp.sum(earlier * onehot, axis=1).reshape(route.shape)
    return route * capacity + ranks


def fill_slots(targets, slot_total, filler):
    token_ids = jnp.repeat(jnp.arange(filler, dtype=jnp.int32), targets.shape[1])
    return jnp.full((slot_total,), filler, jnp.int32).at[targets.reshape(-1)].set(token_ids)


def expert_hidden(rows, weight_gate, weight_up):
    gate_val = jnp.dot(rows, weight_gate, preferred_element_type=jnp.float32)
    up_val = jnp.dot(rows, weight_up, preferred_element_type=jnp.float32)
    return (jax.nn.silu(gate_val) * up_val).astype(jnp.bfloat16)


def per_device(
    conv_x,
    conv_c,
    conv_b,
    conv_taps,
    w_out,
    tokens_b,
    norm_gain,
    route_b,
    route_weights,
    w_gate,
    w_up,
    w_down,
):
    rows_mix = conv_x.shape[0]
    reach_rows = conv_taps.shape[0] - 1
    mixed_u = (conv_c.astype(jnp.float32) * conv_x.astype(jnp.float32)).astype(jnp.bfloat16)
    before = shifted(mixed_u[rows_mix - reach_rows :], ("ep", "tp"), 1)
    extended = jnp.concatenate([before, mixed_u], axis=0)
    filtered = jnp.zeros(mixed_u.shape, jnp.float32)
    for shift_tap in range(reach_rows + 1):
        filtered = filtered + conv_taps[shift_tap][None, :] * extended[
            shift_tap : shift_tap + rows_mix
        ].astype(jnp.float32)
    gated_rows = (conv_b.astype(jnp.float32) * filtered).astype(jnp.bfloat16)
    mixed_out = jnp.dot(
        gated_rows,
        lax.all_gather(w_out, "tp", axis=0, tiled=True),
        preferred_element_type=jnp.float32,
    )
    mixed_a = mixed_out.astype(jnp.bfloat16)
    tokens_f = tokens_b.astype(jnp.float32)
    normed = (
        tokens_f
        * lax.rsqrt(jnp.mean(tokens_f * tokens_f, axis=-1, keepdims=True) + 1e-06)
        * norm_gain
    ).astype(jnp.bfloat16)
    experts = lax.axis_size("ep")
    rows_exp = route_b.shape[0]
    capacity = 2 * rows_exp * TOPK // experts
    slot_total = experts * capacity
    targets = slot_targets(route_b, experts, capacity)
    weight_gate = w_gate[0]
    weight_up = w_up[0]
    weight_down = w_down[0]
    padded_rows = jnp.concatenate([normed, jnp.zeros((1, D), jnp.bfloat16)], axis=0)
    outgoing = padded_rows[fill_slots(targets, slot_total, rows_exp)]
    arrived = lax.all_to_all(outgoing, "ep", split_axis=0, concat_axis=0, tiled=True)
    hidden = expert_hidden(
        lax.all_gather(arrived, "tp", axis=0, tiled=True), weight_gate, weight_up
    )
    summed = lax.psum_scatter(
        jnp.dot(hidden, weight_down, preferred_element_type=jnp.float32).astype(jnp.bfloat16),
        "tp",
        scatter_dimension=0,
        tiled=True,
    )
    returned = lax.all_to_all(summed, "ep", split_axis=0, concat_axis=0, tiled=True)
    picked = returned[targets]
    shares = route_weights / jnp.sum(route_weights, axis=-1, keepdims=True)
    experts_b = jnp.sum(picked.astype(jnp.float32) * shares[:, :, None], axis=1).astype(
        jnp.bfloat16
    )
    return (mixed_a, experts_b)


def swapped(x, axis, mask):
    return lax.ppermute(x, axis, [(i, i ^ mask) for i in range(lax.axis_size(axis))])


def turned(x, axis, by):
    size = lax.axis_size(axis)
    return lax.ppermute(x, axis, [(i, (i + by) % size) for i in range(size)])


def gathered_pieces(w_out):
    me = lax.axis_index("tp")
    grp = lax.axis_index("grp")
    rows = w_out.shape[0]
    half = rows // 2
    mine = lax.dynamic_slice_in_dim(w_out, grp * half, half, axis=0)
    far_mine = swapped(mine, "tp", 2)
    far_other = swapped(far_mine, "grp", 1)
    near = swapped(w_out, "tp", 1)
    diag_mine = swapped(far_mine, "tp", 1)
    diag_other = swapped(far_other, "tp", 1)
    return [
        (me * rows, w_out),
        ((me ^ 1) * rows, near),
        ((me ^ 2) * rows + grp * half, far_mine),
        ((me ^ 3) * rows + grp * half, diag_mine),
        ((me ^ 2) * rows + (1 - grp) * half, far_other),
        ((me ^ 3) * rows + (1 - grp) * half, diag_other),
    ]


def dense_per_device(
    conv_x,
    conv_c,
    conv_b,
    conv_taps,
    w_out,
    tokens_b,
    norm_gain,
    route_b,
    route_weights,
    w_gate,
    w_up,
    w_down,
):
    n_ep = lax.axis_size("ep")
    n_tp = lax.axis_size("tp")
    my_ep = lax.axis_index("ep")
    my_tp = lax.axis_index("tp")
    rows_exp = route_b.shape[0]
    pieces = gathered_pieces(w_out)
    tokens_f = tokens_b.astype(jnp.float32)
    normed = (
        tokens_f
        * lax.rsqrt(jnp.mean(tokens_f * tokens_f, axis=-1, keepdims=True) + 1e-06)
        * norm_gain
    ).astype(jnp.bfloat16)
    shares = route_weights / jnp.sum(route_weights, axis=-1, keepdims=True)
    named = route_b[:, :, None] == jnp.arange(n_ep, dtype=jnp.int32)[None, None, :]
    spread = jnp.sum(jnp.where(named, shares[:, :, None], 0.0), axis=1)
    all_shares = lax.all_gather(spread.T, ("ep", "tp"), axis=0).reshape(
        n_ep, n_tp, n_ep, rows_exp
    )
    expert_shares = lax.dynamic_index_in_dim(all_shares, my_ep, axis=2, keepdims=False)

    rows_mix = conv_x.shape[0]
    reach_rows = conv_taps.shape[0] - 1
    mixed_u = (conv_c.astype(jnp.float32) * conv_x.astype(jnp.float32)).astype(jnp.bfloat16)
    before = shifted(mixed_u[rows_mix - reach_rows :], ("ep", "tp"), 1)
    extended = jnp.concatenate([before, mixed_u], axis=0)
    filtered = jnp.zeros(mixed_u.shape, jnp.float32)
    for shift_tap in range(reach_rows + 1):
        filtered = filtered + conv_taps[shift_tap][None, :] * extended[
            shift_tap : shift_tap + rows_mix
        ].astype(jnp.float32)
    gated_rows = (conv_b.astype(jnp.float32) * filtered).astype(jnp.bfloat16)
    mixed_out = None
    for first, piece in pieces:
        part = jnp.dot(
            lax.dynamic_slice_in_dim(gated_rows, first, piece.shape[0], axis=1),
            piece,
            preferred_element_type=jnp.float32,
        )
        mixed_out = part if mixed_out is None else mixed_out + part
    mixed_a = mixed_out.astype(jnp.bfloat16)

    weight_gate = w_gate[0]
    weight_up = w_up[0]
    weight_down = w_down[0]
    held = normed
    total = None
    for back in range(n_ep):
        if back:
            held = turned(held, "ep", 1)
        far = swapped(held, "tp", 2)
        rows = jnp.concatenate([held, far, swapped(held, "tp", 1), swapped(far, "tp", 1)], axis=0)
        chunk_shares = lax.dynamic_index_in_dim(
            expert_shares, (my_ep - back) % n_ep, axis=0, keepdims=False
        )
        factor = jnp.concatenate(
            [
                lax.dynamic_index_in_dim(chunk_shares, my_tp ^ mask, axis=0, keepdims=False)
                for mask in (0, 2, 1, 3)
            ]
        )
        hidden = expert_hidden(rows, weight_gate, weight_up)
        partial = (
            jnp.dot(hidden, weight_down, preferred_element_type=jnp.float32) * factor[:, None]
        ).astype(jnp.bfloat16)
        lane = 2 * rows_exp
        from_near = swapped(partial[lane:], "tp", 1)
        pair = (
            partial[:lane].astype(jnp.float32) + from_near.astype(jnp.float32)
        ).astype(jnp.bfloat16)
        from_far = swapped(pair[rows_exp:], "tp", 2)
        summed = (
            pair[:rows_exp].astype(jnp.float32) + from_far.astype(jnp.float32)
        ).astype(jnp.bfloat16)
        if back:
            summed = turned(summed, "ep", -back)
        total = (
            summed.astype(jnp.float32) if total is None else total + summed.astype(jnp.float32)
        )
    return (mixed_a, total.astype(jnp.bfloat16))


def planned(mesh):
    def body(*args):
        experts = mesh.shape["ep"]
        rows_exp = args[7].shape[0]
        capacity = 2 * rows_exp * TOPK // experts
        dense = capacity >= rows_exp and mesh.shape["tp"] == 4 and mesh.shape["grp"] == 2
        return (dense_per_device if dense else per_device)(*args)

    return body


def solution(mesh):
    return jax.shard_map(
        planned(mesh),
        mesh=mesh,
        in_specs=(
            P(("grp", "ep", "tp"), None),
            P(("grp", "ep", "tp"), None),
            P(("grp", "ep", "tp"), None),
            P(),
            P("tp", None),
            P(("grp", "ep", "tp"), None),
            P(),
            P(("grp", "ep", "tp"), None),
            P(("grp", "ep", "tp"), None),
            P("ep", None, "tp"),
            P("ep", None, "tp"),
            P("ep", "tp", None),
        ),
        out_specs=(P(("grp", "ep", "tp"), None), P(("grp", "ep", "tp"), None)),
        check_vma=False,
    )
```

```python
import jax
import jax.numpy as jnp
from jax import lax
from jax.sharding import PartitionSpec as P

D = 2048
TOPK = 2


def shifted(x, axis, by):
    size = lax.axis_size(axis)
    pairs = [(i, i + by) for i in range(size) if 0 <= i + by < size]
    return lax.ppermute(x, axis, pairs)


def slot_targets(route, experts, capacity):
    flat = route.reshape(-1)
    onehot = (flat[:, None] == jnp.arange(experts, dtype=jnp.int32)[None, :]).astype(jnp.int32)
    earlier = jnp.cumsum(onehot, axis=0) - onehot
    ranks = jnp.sum(earlier * onehot, axis=1).reshape(route.shape)
    return route * capacity + ranks


def fill_slots(targets, slot_total, filler):
    token_ids = jnp.repeat(jnp.arange(filler, dtype=jnp.int32), targets.shape[1])
    return jnp.full((slot_total,), filler, jnp.int32).at[targets.reshape(-1)].set(token_ids)


def expert_hidden(rows, weight_gate, weight_up):
    gate_val = jnp.dot(rows, weight_gate, preferred_element_type=jnp.float32)
    up_val = jnp.dot(rows, weight_up, preferred_element_type=jnp.float32)
    return (jax.nn.silu(gate_val) * up_val).astype(jnp.bfloat16)


def per_device(
    conv_x,
    conv_c,
    conv_b,
    conv_taps,
    w_out,
    tokens_b,
    norm_gain,
    route_b,
    route_weights,
    w_gate,
    w_up,
    w_down,
):
    rows_mix = conv_x.shape[0]
    reach_rows = conv_taps.shape[0] - 1
    mixed_u = (conv_c.astype(jnp.float32) * conv_x.astype(jnp.float32)).astype(jnp.bfloat16)
    before = shifted(mixed_u[rows_mix - reach_rows :], ("ep", "tp"), 1)
    extended = jnp.concatenate([before, mixed_u], axis=0)
    filtered = jnp.zeros(mixed_u.shape, jnp.float32)
    for shift_tap in range(reach_rows + 1):
        filtered = filtered + conv_taps[shift_tap][None, :] * extended[
            shift_tap : shift_tap + rows_mix
        ].astype(jnp.float32)
    gated_rows = (conv_b.astype(jnp.float32) * filtered).astype(jnp.bfloat16)
    mixed_out = jnp.dot(
        gated_rows,
        lax.all_gather(w_out, "tp", axis=0, tiled=True),
        preferred_element_type=jnp.float32,
    )
    mixed_a = mixed_out.astype(jnp.bfloat16)
    tokens_f = tokens_b.astype(jnp.float32)
    normed = (
        tokens_f
        * lax.rsqrt(jnp.mean(tokens_f * tokens_f, axis=-1, keepdims=True) + 1e-06)
        * norm_gain
    ).astype(jnp.bfloat16)
    experts = lax.axis_size("ep")
    rows_exp = route_b.shape[0]
    capacity = 2 * rows_exp * TOPK // experts
    slot_total = experts * capacity
    targets = slot_targets(route_b, experts, capacity)
    weight_gate = w_gate[0]
    weight_up = w_up[0]
    weight_down = w_down[0]
    padded_rows = jnp.concatenate([normed, jnp.zeros((1, D), jnp.bfloat16)], axis=0)
    outgoing = padded_rows[fill_slots(targets, slot_total, rows_exp)]
    arrived = lax.all_to_all(outgoing, "ep", split_axis=0, concat_axis=0, tiled=True)
    hidden = expert_hidden(
        lax.all_gather(arrived, "tp", axis=0, tiled=True), weight_gate, weight_up
    )
    summed = lax.psum_scatter(
        jnp.dot(hidden, weight_down, preferred_element_type=jnp.float32).astype(jnp.bfloat16),
        "tp",
        scatter_dimension=0,
        tiled=True,
    )
    returned = lax.all_to_all(summed, "ep", split_axis=0, concat_axis=0, tiled=True)
    picked = returned[targets]
    shares = route_weights / jnp.sum(route_weights, axis=-1, keepdims=True)
    experts_b = jnp.sum(picked.astype(jnp.float32) * shares[:, :, None], axis=1).astype(
        jnp.bfloat16
    )
    return (mixed_a, experts_b)


def swapped(x, axis, mask):
    return lax.ppermute(x, axis, [(i, i ^ mask) for i in range(lax.axis_size(axis))])


def turned(x, axis, by):
    size = lax.axis_size(axis)
    return lax.ppermute(x, axis, [(i, (i + by) % size) for i in range(size)])


def gathered_pieces(w_out):
    me = lax.axis_index("tp")
    grp = lax.axis_index("grp")
    rows = w_out.shape[0]
    half = rows // 2
    mine = lax.dynamic_slice_in_dim(w_out, grp * half, half, axis=0)
    far_mine = swapped(mine, "tp", 2)
    far_other = swapped(far_mine, "grp", 1)
    near = swapped(w_out, "tp", 1)
    diag_mine = swapped(far_mine, "tp", 1)
    diag_other = swapped(far_other, "tp", 1)
    return [
        (me * rows, w_out),
        ((me ^ 1) * rows, near),
        ((me ^ 2) * rows + grp * half, far_mine),
        ((me ^ 3) * rows + grp * half, diag_mine),
        ((me ^ 2) * rows + (1 - grp) * half, far_other),
        ((me ^ 3) * rows + (1 - grp) * half, diag_other),
    ]


def dense_per_device(
    conv_x,
    conv_c,
    conv_b,
    conv_taps,
    w_out,
    tokens_b,
    norm_gain,
    route_b,
    route_weights,
    w_gate,
    w_up,
    w_down,
):
    n_ep = lax.axis_size("ep")
    my_ep = lax.axis_index("ep")
    rows_exp = route_b.shape[0]
    pieces = gathered_pieces(w_out)
    tokens_f = tokens_b.astype(jnp.float32)
    normed = (
        tokens_f
        * lax.rsqrt(jnp.mean(tokens_f * tokens_f, axis=-1, keepdims=True) + 1e-06)
        * norm_gain
    ).astype(jnp.bfloat16)
    shares = route_weights / jnp.sum(route_weights, axis=-1, keepdims=True)

    rows_mix = conv_x.shape[0]
    reach_rows = conv_taps.shape[0] - 1
    mixed_u = (conv_c.astype(jnp.float32) * conv_x.astype(jnp.float32)).astype(jnp.bfloat16)
    before = shifted(mixed_u[rows_mix - reach_rows :], ("ep", "tp"), 1)
    extended = jnp.concatenate([before, mixed_u], axis=0)
    filtered = jnp.zeros(mixed_u.shape, jnp.float32)
    for shift_tap in range(reach_rows + 1):
        filtered = filtered + conv_taps[shift_tap][None, :] * extended[
            shift_tap : shift_tap + rows_mix
        ].astype(jnp.float32)
    gated_rows = (conv_b.astype(jnp.float32) * filtered).astype(jnp.bfloat16)
    mixed_out = None
    for first, piece in pieces:
        part = jnp.dot(
            lax.dynamic_slice_in_dim(gated_rows, first, piece.shape[0], axis=1),
            piece,
            preferred_element_type=jnp.float32,
        )
        mixed_out = part if mixed_out is None else mixed_out + part
    mixed_a = mixed_out.astype(jnp.bfloat16)

    weight_gate = w_gate[0]
    weight_up = w_up[0]
    weight_down = w_down[0]

    def expert(rows):
        return jnp.dot(
            expert_hidden(rows, weight_gate, weight_up),
            weight_down,
            preferred_element_type=jnp.float32,
        )

    helds = [normed]
    for back in range(1, n_ep):
        helds.append(turned(helds[-1], "ep", 1))
    order = [*range(1, n_ep), 0]
    if n_ep > 2:
        helds[0], helds[2] = lax.optimization_barrier((helds[0], helds[2]))
    pairs, sums, backs = [], [], []
    for at, back in enumerate(order):
        held = helds[back]
        lane = jnp.concatenate([held, swapped(held, "tp", 2)], axis=0)
        near = swapped(lane, "tp", 1)
        if at >= 1:
            near, pairs[at - 1] = lax.optimization_barrier((near, pairs[at - 1]))
            from_far = swapped(pairs[at - 1][rows_exp:], "tp", 2)
            sums.append(
                (
                    pairs[at - 1][:rows_exp].astype(jnp.float32) + from_far.astype(jnp.float32)
                ).astype(jnp.bfloat16)
            )
        if at >= 2:
            near, sums[at - 2] = lax.optimization_barrier((near, sums[at - 2]))
            backs.append(turned(sums[at - 2], "ep", -order[at - 2]))
        from_near = swapped(expert(near).astype(jnp.bfloat16), "tp", 1)
        pairs.append((expert(lane) + from_near.astype(jnp.float32)).astype(jnp.bfloat16))
    last, *backs = lax.optimization_barrier((pairs[-1], *backs))
    from_far = swapped(last[rows_exp:], "tp", 2)
    sums.append(
        (last[:rows_exp].astype(jnp.float32) + from_far.astype(jnp.float32)).astype(jnp.bfloat16)
    )
    for at in range(len(backs), n_ep):
        backs.append(turned(sums[at], "ep", -order[at]) if order[at] else sums[at])
    total = jnp.zeros((rows_exp, D), jnp.float32)
    for back, summed in zip(order, backs):
        chosen = route_b == (my_ep + back) % n_ep
        share = jnp.sum(jnp.where(chosen, shares, 0.0), axis=1, keepdims=True)
        total = total + summed.astype(jnp.float32) * share
    return (mixed_a, total.astype(jnp.bfloat16))


def planned(mesh):
    def body(*args):
        experts = mesh.shape["ep"]
        rows_exp = args[7].shape[0]
        capacity = 2 * rows_exp * TOPK // experts
        dense = capacity >= rows_exp and mesh.shape["tp"] == 4 and mesh.shape["grp"] == 2
        return (dense_per_device if dense else per_device)(*args)

    return body


def solution(mesh):
    return jax.shard_map(
        planned(mesh),
        mesh=mesh,
        in_specs=(
            P(("grp", "ep", "tp"), None),
            P(("grp", "ep", "tp"), None),
            P(("grp", "ep", "tp"), None),
            P(),
            P("tp", None),
            P(("grp", "ep", "tp"), None),
            P(),
            P(("grp", "ep", "tp"), None),
            P(("grp", "ep", "tp"), None),
            P("ep", None, "tp"),
            P("ep", None, "tp"),
            P("ep", "tp", None),
        ),
        out_specs=(P(("grp", "ep", "tp"), None), P(("grp", "ep", "tp"), None)),
        check_vma=False,
    )
```

```python
import jax
import jax.numpy as jnp
from jax import lax
from jax.sharding import PartitionSpec as P

D = 2048
TOPK = 2


def shifted(x, axis, by):
    size = lax.axis_size(axis)
    pairs = [(i, i + by) for i in range(size) if 0 <= i + by < size]
    return lax.ppermute(x, axis, pairs)


def slot_targets(route, experts, capacity):
    flat = route.reshape(-1)
    onehot = (flat[:, None] == jnp.arange(experts, dtype=jnp.int32)[None, :]).astype(jnp.int32)
    earlier = jnp.cumsum(onehot, axis=0) - onehot
    ranks = jnp.sum(earlier * onehot, axis=1).reshape(route.shape)
    return route * capacity + ranks


def fill_slots(targets, slot_total, filler):
    token_ids = jnp.repeat(jnp.arange(filler, dtype=jnp.int32), targets.shape[1])
    return jnp.full((slot_total,), filler, jnp.int32).at[targets.reshape(-1)].set(token_ids)


def expert_hidden(rows, weight_gate, weight_up):
    gate_val = jnp.dot(rows, weight_gate, preferred_element_type=jnp.float32)
    up_val = jnp.dot(rows, weight_up, preferred_element_type=jnp.float32)
    return (jax.nn.silu(gate_val) * up_val).astype(jnp.bfloat16)


def per_device(
    conv_x,
    conv_c,
    conv_b,
    conv_taps,
    w_out,
    tokens_b,
    norm_gain,
    route_b,
    route_weights,
    w_gate,
    w_up,
    w_down,
):
    rows_mix = conv_x.shape[0]
    reach_rows = conv_taps.shape[0] - 1
    mixed_u = (conv_c.astype(jnp.float32) * conv_x.astype(jnp.float32)).astype(jnp.bfloat16)
    before = shifted(mixed_u[rows_mix - reach_rows :], ("ep", "tp"), 1)
    extended = jnp.concatenate([before, mixed_u], axis=0)
    filtered = jnp.zeros(mixed_u.shape, jnp.float32)
    for shift_tap in range(reach_rows + 1):
        filtered = filtered + conv_taps[shift_tap][None, :] * extended[
            shift_tap : shift_tap + rows_mix
        ].astype(jnp.float32)
    gated_rows = (conv_b.astype(jnp.float32) * filtered).astype(jnp.bfloat16)
    mixed_out = jnp.dot(
        gated_rows,
        lax.all_gather(w_out, "tp", axis=0, tiled=True),
        preferred_element_type=jnp.float32,
    )
    mixed_a = mixed_out.astype(jnp.bfloat16)
    tokens_f = tokens_b.astype(jnp.float32)
    normed = (
        tokens_f
        * lax.rsqrt(jnp.mean(tokens_f * tokens_f, axis=-1, keepdims=True) + 1e-06)
        * norm_gain
    ).astype(jnp.bfloat16)
    experts = lax.axis_size("ep")
    rows_exp = route_b.shape[0]
    capacity = 2 * rows_exp * TOPK // experts
    slot_total = experts * capacity
    targets = slot_targets(route_b, experts, capacity)
    weight_gate = w_gate[0]
    weight_up = w_up[0]
    weight_down = w_down[0]
    padded_rows = jnp.concatenate([normed, jnp.zeros((1, D), jnp.bfloat16)], axis=0)
    outgoing = padded_rows[fill_slots(targets, slot_total, rows_exp)]
    arrived = lax.all_to_all(outgoing, "ep", split_axis=0, concat_axis=0, tiled=True)
    hidden = expert_hidden(
        lax.all_gather(arrived, "tp", axis=0, tiled=True), weight_gate, weight_up
    )
    summed = lax.psum_scatter(
        jnp.dot(hidden, weight_down, preferred_element_type=jnp.float32).astype(jnp.bfloat16),
        "tp",
        scatter_dimension=0,
        tiled=True,
    )
    returned = lax.all_to_all(summed, "ep", split_axis=0, concat_axis=0, tiled=True)
    picked = returned[targets]
    shares = route_weights / jnp.sum(route_weights, axis=-1, keepdims=True)
    experts_b = jnp.sum(picked.astype(jnp.float32) * shares[:, :, None], axis=1).astype(
        jnp.bfloat16
    )
    return (mixed_a, experts_b)


def swapped(x, axis, mask):
    return lax.ppermute(x, axis, [(i, i ^ mask) for i in range(lax.axis_size(axis))])


def turned(x, axis, by):
    size = lax.axis_size(axis)
    return lax.ppermute(x, axis, [(i, (i + by) % size) for i in range(size)])


def gathered_pieces(w_out, helds):
    me = lax.axis_index("tp")
    grp = lax.axis_index("grp")
    rows = w_out.shape[0]
    half = rows // 2
    mine = lax.dynamic_slice_in_dim(w_out, grp * half, half, axis=0)
    if len(helds) > 2:
        mine, helds[2] = lax.optimization_barrier((mine, helds[2]))
    far_mine = swapped(mine, "tp", 2)
    far_other = swapped(far_mine, "grp", 1)
    near = swapped(w_out, "tp", 1)
    diag_mine = swapped(far_mine, "tp", 1)
    diag_other = swapped(far_other, "tp", 1)
    return [
        (me * rows, w_out),
        ((me ^ 1) * rows, near),
        ((me ^ 2) * rows + grp * half, far_mine),
        ((me ^ 3) * rows + grp * half, diag_mine),
        ((me ^ 2) * rows + (1 - grp) * half, far_other),
        ((me ^ 3) * rows + (1 - grp) * half, diag_other),
    ]


def dense_per_device(
    conv_x,
    conv_c,
    conv_b,
    conv_taps,
    w_out,
    tokens_b,
    norm_gain,
    route_b,
    route_weights,
    w_gate,
    w_up,
    w_down,
):
    n_ep = lax.axis_size("ep")
    my_ep = lax.axis_index("ep")
    rows_exp = route_b.shape[0]
    tokens_f = tokens_b.astype(jnp.float32)
    normed = (
        tokens_f
        * lax.rsqrt(jnp.mean(tokens_f * tokens_f, axis=-1, keepdims=True) + 1e-06)
        * norm_gain
    ).astype(jnp.bfloat16)
    helds = [normed]
    for back in range(1, n_ep):
        helds.append(turned(helds[-1], "ep", 1))
    pieces = gathered_pieces(w_out, helds)
    shares = route_weights / jnp.sum(route_weights, axis=-1, keepdims=True)

    rows_mix = conv_x.shape[0]
    reach_rows = conv_taps.shape[0] - 1
    mixed_u = (conv_c.astype(jnp.float32) * conv_x.astype(jnp.float32)).astype(jnp.bfloat16)
    before = shifted(mixed_u[rows_mix - reach_rows :], ("ep", "tp"), 1)
    extended = jnp.concatenate([before, mixed_u], axis=0)
    filtered = jnp.zeros(mixed_u.shape, jnp.float32)
    for shift_tap in range(reach_rows + 1):
        filtered = filtered + conv_taps[shift_tap][None, :] * extended[
            shift_tap : shift_tap + rows_mix
        ].astype(jnp.float32)
    gated_rows = (conv_b.astype(jnp.float32) * filtered).astype(jnp.bfloat16)
    mixed_out = None
    for first, piece in pieces:
        part = jnp.dot(
            lax.dynamic_slice_in_dim(gated_rows, first, piece.shape[0], axis=1),
            piece,
            preferred_element_type=jnp.float32,
        )
        mixed_out = part if mixed_out is None else mixed_out + part
    mixed_a = mixed_out.astype(jnp.bfloat16)

    weight_gate = w_gate[0]
    weight_up = w_up[0]
    weight_down = w_down[0]

    def expert(rows):
        return jnp.dot(
            expert_hidden(rows, weight_gate, weight_up),
            weight_down,
            preferred_element_type=jnp.float32,
        )

    order = [*range(1, n_ep), 0]
    pairs, sums, backs = [], [], []
    for at, back in enumerate(order):
        held = helds[back]
        lane = jnp.concatenate([held, swapped(held, "tp", 2)], axis=0)
        near = swapped(lane, "tp", 1)
        if at >= 1:
            near, pairs[at - 1], *backs = lax.optimization_barrier((near, pairs[at - 1], *backs))
            from_far = swapped(pairs[at - 1][rows_exp:], "tp", 2)
            sums.append(
                (
                    pairs[at - 1][:rows_exp].astype(jnp.float32) + from_far.astype(jnp.float32)
                ).astype(jnp.bfloat16)
            )
        if at >= 2:
            near, sums[at - 2] = lax.optimization_barrier((near, sums[at - 2]))
            backs.append(turned(sums[at - 2], "ep", -order[at - 2]))
        from_near = swapped(expert(near).astype(jnp.bfloat16), "tp", 1)
        pairs.append((expert(lane) + from_near.astype(jnp.float32)).astype(jnp.bfloat16))
    last, *backs = lax.optimization_barrier((pairs[-1], *backs))
    from_far = swapped(last[rows_exp:], "tp", 2)
    sums.append(
        (last[:rows_exp].astype(jnp.float32) + from_far.astype(jnp.float32)).astype(jnp.bfloat16)
    )
    for at in range(len(backs), n_ep):
        backs.append(turned(sums[at], "ep", -order[at]) if order[at] else sums[at])
    total = jnp.zeros((rows_exp, D), jnp.float32)
    for back, summed in zip(order, backs):
        chosen = route_b == (my_ep + back) % n_ep
        share = jnp.sum(jnp.where(chosen, shares, 0.0), axis=1, keepdims=True)
        total = total + summed.astype(jnp.float32) * share
    return (mixed_a, total.astype(jnp.bfloat16))


def planned(mesh):
    def body(*args):
        experts = mesh.shape["ep"]
        rows_exp = args[7].shape[0]
        capacity = 2 * rows_exp * TOPK // experts
        dense = capacity >= rows_exp and mesh.shape["tp"] == 4 and mesh.shape["grp"] == 2
        return (dense_per_device if dense else per_device)(*args)

    return body


def solution(mesh):
    return jax.shard_map(
        planned(mesh),
        mesh=mesh,
        in_specs=(
            P(("grp", "ep", "tp"), None),
            P(("grp", "ep", "tp"), None),
            P(("grp", "ep", "tp"), None),
            P(),
            P("tp", None),
            P(("grp", "ep", "tp"), None),
            P(),
            P(("grp", "ep", "tp"), None),
            P(("grp", "ep", "tp"), None),
            P("ep", None, "tp"),
            P("ep", None, "tp"),
            P("ep", "tp", None),
        ),
        out_specs=(P(("grp", "ep", "tp"), None), P(("grp", "ep", "tp"), None)),
        check_vma=False,
    )
```
